32 devices in a mesh: sp: 4 (over z), dp: 8 (over y, x, core).
Axes of the slice: x: 2, y: 2, z: 4, core: 2. Of those that a mesh axis runs over, the one named last changes fastest.
Arguments:
- stream_x: bfloat16 [8, 512, 2048], P('dp', 'sp'), may hold values from -6 to 6
- stream_b: bfloat16 [8, 512, 1024], P('dp', 'sp'), may hold values from -6 to 6
- stream_c: bfloat16 [8, 512, 1024], P('dp', 'sp'), may hold values from -6 to 6
- gate_z: bfloat16 [8, 512, 2048], P('dp', 'sp'), may hold values from -6 to 6
- step_raw: bfloat16 [8, 512, 32], P('dp', 'sp'), may hold values from -4 to 3
- conv_x: bfloat16 [4, 2048], P(None, 'sp'), may hold values from -3 to 3
- conv_b: bfloat16 [4, 1024], replicated, may hold values from -3 to 3
- conv_c: bfloat16 [4, 1024], replicated, may hold values from -3 to 3
- decay_log: float32 [32], P('sp'), may hold values from -20 to 0
- norm_gain: float32 [2048], replicated, may hold values from 0.1 to 1.9
- w_out: bfloat16 [2048, 2048], P('dp'), may hold values from -0.125 to 0.125
Outputs:
- mixed: bfloat16 [8, 512, 2048], P('dp', 'sp')
The draws below stay inside these ranges and needn't reach their ends.
All inputs are finite; a program needn't handle non-finite values.
Results may differ from the reference program's by a relative error of at most 0.011.
Values may be sent and summed in bfloat16 or wider, within the bound.
A program may use at most 64 MiB of HBM per device.

```python
import jax
import jax.numpy as jnp
from jax import lax

D = 2048
HEADS = 32
HEAD_DIM = 64
STATE = 128
CONV = 4
BLOCK = 64
TOK_DEV = 128
DI = 2048
GROUP_STATE = 1024
SEQS = 8
LEN = 512


def draw_step_raw(key, part):
    first_key, second_key = jax.random.split(jax.random.fold_in(key, 11))
    noise = jnp.clip(jax.random.normal(first_key, (SEQS, LEN, HEADS), jnp.float32), -3.0, 3.0)
    offset = jax.random.uniform(second_key, (SEQS, LEN // TOK_DEV, 1, HEADS), jnp.float32, -2.0, 1.0)
    offset = jnp.broadcast_to(offset, (SEQS, LEN // TOK_DEV, TOK_DEV, HEADS)).reshape(SEQS, LEN, HEADS)
    return (0.6 * noise + offset).astype(jnp.bfloat16)


def draw_decay_log(key, part):
    pick_key, slow_key, quick_key = jax.random.split(jax.random.fold_in(key, 23), 3)
    chance = 0.5
    quick_heads = jax.random.uniform(pick_key, (HEADS,), jnp.float32) < chance
    slow_rate = jax.random.uniform(slow_key, (HEADS,), jnp.float32, 0.3, 1.0) / LEN
    quick_rate = jax.random.uniform(quick_key, (HEADS,), jnp.float32, 0.03, 0.08)
    return jnp.log(jnp.where(quick_heads, quick_rate, slow_rate)).astype(jnp.float32)


def shard_levels(key, dims, cuts, least, largest):
    factor_of, own = 1.0, jax.random.fold_in(key, 6)
    for position, blocks in cuts:
        heights = jnp.exp(jax.random.uniform(jax.random.fold_in(own, position), (blocks,), jnp.float32, least / len(cuts), largest / len(cuts)))
        factor_of = factor_of * jnp.repeat(heights, dims[position] // blocks).reshape([-1 if axis == position else 1 for axis in range(len(dims))])
    return factor_of


def scatter_about(own_key, extent, scale, limit, shards=(), dtype=jnp.bfloat16):
    factor_of = shard_levels(own_key, extent, shards, -0.22, 0.18) if shards else 1.0
    drawn = jax.random.normal(own_key, extent, jnp.float32) * scale * factor_of
    return jnp.minimum(jnp.maximum(drawn, -limit), limit).astype(dtype)


def setup_inputs(seed: int = 0) -> dict:
    seeds = jax.random.split(jax.random.key(seed), 12)
    return {
        "stream_x": scatter_about(seeds[0], (SEQS, LEN, DI), 1.0, 6.0, ((0, 8), (1, 4))),
        "stream_b": scatter_about(seeds[1], (SEQS, LEN, GROUP_STATE), 1.0, 6.0, ((0, 8), (1, 4))),
        "stream_c": scatter_about(seeds[2], (SEQS, LEN, GROUP_STATE), 1.0, 6.0, ((0, 8), (1, 4))),
        "gate_z": scatter_about(seeds[3], (SEQS, LEN, DI), 1.0, 6.0, ((0, 8), (1, 4))),
        "step_raw": draw_step_raw(jax.random.fold_in(seeds[11], 71), 0),
        "conv_x": scatter_about(seeds[5], (CONV, DI), CONV ** -0.5, 3.0, ((1, 4),)),
        "conv_b": scatter_about(seeds[6], (CONV, GROUP_STATE), CONV ** -0.5, 3.0),
        "conv_c": scatter_about(seeds[7], (CONV, GROUP_STATE), CONV ** -0.5, 3.0),
        "decay_log": draw_decay_log(jax.random.fold_in(seeds[11], 71), 0),
        "norm_gain": jnp.clip(1.0 + 0.18 * jax.random.normal(seeds[9], (DI,), jnp.float32), 0.1, 1.9),
        "w_out": scatter_about(seeds[10], (DI, D), DI ** -0.5, 0.125, ((0, 8),)),
    }


NORM_EPS = 1.0

def causal_conv(sequence, kernel):
    taps = kernel.shape[0]
    length = sequence.shape[0]
    padded = jnp.pad(sequence.astype(jnp.float32), ((taps - 1, 0), (0, 0)))
    summed = jnp.zeros(sequence.shape, jnp.float32)
    for tap_index in range(taps):
        summed = summed + kernel[tap_index].astype(jnp.float32) * padded[tap_index:tap_index + length]
    rounded = lax.optimization_barrier(jax.nn.silu(summed).astype(jnp.bfloat16))
    return rounded.astype(jnp.float32)

def mixer(seq_x, seq_b, seq_c, seq_raw, conv_x, conv_b, conv_c, decay_log):
    length = seq_x.shape[0]
    head_count = seq_raw.shape[1]
    group_count = seq_b.shape[1] // STATE
    ratio = head_count // group_count
    blocks = length // BLOCK
    highest = lax.Precision.HIGHEST
    x_values = causal_conv(seq_x, conv_x).reshape(blocks, BLOCK, group_count, ratio, HEAD_DIM)
    b_values = causal_conv(seq_b, conv_b).reshape(blocks, BLOCK, group_count, STATE)
    c_values = causal_conv(seq_c, conv_c).reshape(blocks, BLOCK, group_count, STATE)
    step_size = jax.nn.softplus(seq_raw.astype(jnp.float32))
    log_decay = (step_size * (-jnp.exp(decay_log))[None, :]).reshape(blocks, BLOCK, group_count, ratio)
    step_size = step_size.reshape(blocks, BLOCK, group_count, ratio)
    cumul = jnp.cumsum(log_decay, axis=1)
    scores = jnp.einsum('kTgn,kSgn->kTSg', c_values, b_values, precision=highest)
    causal = jnp.tril(jnp.ones((BLOCK, BLOCK), bool))
    spread = cumul[:, :, None] - cumul[:, None, :]
    decay = jnp.exp(jnp.where(causal[None, :, :, None, None], spread, -jnp.inf))
    weights = scores[..., None] * decay * step_size[:, None]
    inner = jnp.einsum('kTSgr,kSgrp->kTgrp', weights, x_values, precision=highest)
    last = cumul[:, -1]
    tail = jnp.exp(last[:, None] - cumul) * step_size
    local = jnp.einsum('kSgn,kSgr,kSgrp->kgrpn', b_values, tail, x_values, precision=highest)
    before = jnp.cumsum(last, axis=0) - last
    after = before + last
    gap = before[:, None] - after[None, :]
    lower = jnp.tril(jnp.ones((blocks, blocks), bool), -1)
    carry_weight = jnp.exp(jnp.where(lower[:, :, None, None], gap, -jnp.inf))
    entering = jnp.einsum('kjgr,jgrpn->kgrpn', carry_weight, local, precision=highest)
    carried = jnp.einsum('kTgn,kgrpn,kTgr->kTgrp', c_values, entering, jnp.exp(cumul), precision=highest)
    return (inner + carried).reshape(length, head_count * HEAD_DIM).astype(jnp.bfloat16)

def gate_norm(core_out, seq_z, gain, group_width):
    length = core_out.shape[0]
    gated = core_out.astype(jnp.float32) * jax.nn.silu(seq_z.astype(jnp.float32))
    grouped = gated.reshape(length, -1, group_width)
    scale = lax.rsqrt(lax.optimization_barrier(jnp.mean(grouped * grouped, axis=-1, keepdims=True)) + NORM_EPS)
    return ((grouped * scale).reshape(length, -1) * gain[None, :]).astype(jnp.bfloat16)

def reference(stream_x, stream_b, stream_c, gate_z, step_raw, conv_x, conv_b, conv_c, decay_log, norm_gain, w_out):
    group_width = HEAD_DIM

    def one_sequence(inputs):
        seq_x, seq_b, seq_c, seq_z, seq_raw = inputs
        core_out = mixer(seq_x, seq_b, seq_c, seq_raw, conv_x, conv_b, conv_c, decay_log)
        normed = gate_norm(core_out, seq_z, norm_gain, group_width)
        return jnp.dot(normed, w_out, preferred_element_type=jnp.float32).astype(jnp.bfloat16)
    return lax.map(one_sequence, (stream_x, stream_b, stream_c, gate_z, step_raw))
```

```python
import functools
import math

import jax
import jax.numpy as jnp
from jax import lax
from jax.experimental import pallas as pl
from jax.experimental.pallas import tpu as pltpu
from jax.sharding import PartitionSpec as P

HEAD_DIM = 64
STATE = 128
NORM_EPS = 1.0
HALO = 16
LAG = 3
FIRST_AT = 7
SHARE_AT = 5
TEAM = 2
LANES = 128
F32 = jnp.float32
BF16 = jnp.bfloat16


def dot(a, b, precision=None):
    return jnp.dot(a, b, preferred_element_type=F32, precision=precision)


def ring_items(sp, chips, half_rows):
    share = chips % 2 == 0 and TEAM > 1 and sp % TEAM == 0 and half_rows % (HALO * TEAM) == 0
    items = [[], []]
    for way in range(2):
        for hop in range(1, (chips - 1) // 2 + 1):
            if share:
                items[way] += [(hop, way, part) for part in range(TEAM)]
            else:
                items[way].append((hop, way, None))
            items[way].append((hop, 1 - way, None))
        if chips % 2 == 0:
            items[way].append((chips // 2, way, 0 if share else None))
    return items, share


def kernel(
    sp,
    dp,
    x_hbm,
    b_hbm,
    c_hbm,
    z_hbm,
    raw_ref,
    cx_hbm,
    cb_hbm,
    cc_hbm,
    dl_ref,
    gain_hbm,
    w_hbm,
    out_ref,
    cx_ref,
    cb_ref,
    cc_ref,
    gain_ref,
    x_v,
    b_v,
    c_v,
    z_v,
    halo_x,
    halo_b,
    halo_c,
    par,
    taps,
    wide_raw,
    ext,
    inner,
    ecum,
    elast,
    cact,
    local,
    s_in,
    s_out,
    normed,
    w_all,
    acc,
    in_sem,
    par_send,
    par_recv,
    halo_send,
    halo_recv,
    chain_send,
    chain_recv,
    own_sem,
    ring_send,
    ring_recv,
    relay_send,
    relay_recv,
    share_send,
    share_recv,
    hand_send,
    hand_recv,
):
    tokens, inner_width = x_v.shape
    groups = b_v.shape[1] // STATE
    group_width = inner_width // groups
    pairs = group_width // LANES
    ratio = group_width // HEAD_DIM
    local_heads = dl_ref.shape[1]
    tap_count, tap_width = cx_ref.shape
    rows = w_hbm.shape[0]
    half_rows = rows // 2
    chips = dp // 2
    side = math.isqrt(chips)
    side = side if side * side == chips else chips

    pos = lax.axis_index("sp")
    me = lax.axis_index("dp")
    core = me % 2
    partner = me + 1 - 2 * core

    def snake(place):
        line = place // side
        column = place % side
        return line * side + column + (line % 2) * (side - 1 - 2 * column)

    ring_at = snake(me // 2)

    def ring_device(offset, which):
        return 2 * snake((ring_at + offset + chips) % chips) + which

    right = ring_device(1, core)
    left = ring_device(-1, core)
    following = (pos + 1) % sp

    def remote(src, dst, send, recv, target):
        return pltpu.make_async_remote_copy(
            src_ref=src,
            dst_ref=dst,
            send_sem=send,
            recv_sem=recv,
            device_id=target,
            device_id_type=pl.DeviceIdType.MESH,
        )

    sources = (
        (cx_hbm, cx_ref),
        (b_hbm.at[0], b_v),
        (c_hbm.at[0], c_v),
        (x_hbm.at[0], x_v),
        (cb_hbm, cb_ref),
        (cc_hbm, cc_ref),
        (z_hbm.at[0], z_v),
        (gain_hbm, gain_ref),
    )
    loads = [
        pltpu.make_async_copy(src, dst, in_sem.at[i]) for i, (src, dst) in enumerate(sources)
    ]
    for load in loads:
        load.start()

    barrier = pltpu.get_barrier_semaphore()
    for target in [{"dp": right}, {"dp": left}, {"dp": partner}] + [
        {"sp": (pos + j) % sp} for j in range(1, sp)
    ]:
        pl.semaphore_signal(
            barrier, inc=1, device_id=target, device_id_type=pl.DeviceIdType.MESH
        )

    def w_rows(device, start, count):
        first = pl.multiple_of(device * rows + start, count)
        return w_all.at[pl.ds(first, count), :]

    keep = pltpu.make_async_copy(w_hbm, w_rows(me, 0, rows), in_sem.at[len(sources)])
    keep.start()

    par[pos] = jnp.zeros(par.shape[1:], F32)
    wide_raw[...] = jnp.zeros(wide_raw.shape, F32)
    wide_raw[0:1, 0:local_heads] = dl_ref[...]
    par[pos, :, tap_width : tap_width + LANES] = pltpu.roll(
        wide_raw[0:8, :], pos * local_heads, 1
    )
    wide_raw[...] = jnp.zeros(wide_raw.shape, F32)
    wide_raw[0 : raw_ref.shape[1], :] = raw_ref[0].astype(F32)
    loads[0].wait()
    par[pos, 0:tap_count, 0:tap_width] = cx_ref[...].astype(F32)
    pl.semaphore_wait(barrier, 2 + sp)

    items, share = ring_items(sp, chips, half_rows)
    quarter = half_rows // TEAM
    mate = pos % TEAM
    far = chips // 2

    def rows_of(half, part):
        if part is None:
            return half * half_rows, half_rows
        return half * half_rows + (mate + part) % TEAM * quarter, quarter

    def ring_copy(way, spot):
        hop, half, part = items[way][spot]
        offset = -(hop - 1) if way == 0 else hop - 1
        origin = ring_device(offset, core)
        start, count = rows_of(half, part)
        place = w_rows(origin, start, count)
        src = w_hbm.at[pl.ds(pl.multiple_of(start, count), count), :] if hop == 1 else place
        return remote(
            src,
            place,
            ring_send.at[way, spot],
            ring_recv.at[way, spot],
            {"dp": right if way == 0 else left},
        )

    def relay_copy(way, spot):
        hop, half, part = items[way][spot]
        offset = -hop if way == 0 else hop
        piece = w_rows(ring_device(offset, core), *rows_of(half, part))
        return remote(
            piece, piece, relay_send.at[way, spot], relay_recv.at[way, spot], {"dp": partner}
        )

    def arrived(way, spot):
        hop, half, part = items[way][spot]
        ring_copy(way, spot).wait_recv()
        if (hop + 1, half, part) in items[way]:
            ring_copy(way, items[way].index((hop + 1, half, part))).start()
        relay_copy(way, spot).start()

    def share_copy(up, way):
        piece = w_rows(ring_device(far, core), way * half_rows + mate * quarter, quarter)
        target = (pos + 1) % sp if up else (pos + sp - 1) % sp
        at = (0 if up else 1, way)
        return remote(piece, piece, share_send.at[at], share_recv.at[at], {"sp": target})

    def share_relay(way):
        piece = w_rows(ring_device(far, core), way * half_rows + (1 - mate) * quarter, quarter)
        return remote(piece, piece, hand_send.at[way], hand_recv.at[way], {"dp": partner})

    def send_shares(up):
        for way in range(2):
            share_copy(up, way).start()

    held_back = []
    for spot in range(len(items[0])):
        for way in range(2):
            hop, half, part = items[way][spot]
            if hop == 1 and share and half != way:
                held_back.append((way, spot))
            elif hop == 1:
                ring_copy(way, spot).start()

    halos = [
        remote(
            src.at[0, pl.ds(tokens - HALO, HALO), :],
            dst,
            halo_send.at[i],
            halo_recv.at[i],
            {"sp": following},
        )
        for i, (src, dst) in enumerate(
            ((x_hbm, halo_x), (b_hbm, halo_b), (c_hbm, halo_c))
        )
    ]

    @pl.when(pos < sp - 1)
    def _():
        for copy in halos:
            copy.start()

    shares = [
        remote(
            par.at[pos],
            par.at[pos],
            par_send.at[j - 1],
            par_recv.at[j - 1],
            {"sp": (pos + j) % sp},
        )
        for j in range(1, sp)
    ]
    for copy in shares:
        copy.start()

    own = remote(w_hbm, w_rows(me, 0, rows), own_sem.at[0], own_sem.at[1], {"dp": partner})
    own.start()

    raw = jnp.transpose(wide_raw[...])
    dt = jnp.maximum(raw, 0.0) + jnp.log(1.0 + jnp.exp(-jnp.abs(raw)))
    down = lax.broadcasted_iota(jnp.int32, (tokens, tokens), 0)
    across = lax.broadcasted_iota(jnp.int32, (tokens, tokens), 1)
    causal = down >= across
    loads[4].wait()
    loads[5].wait()
    for g in range(groups):
        taps[g, 0:tap_count, group_width : group_width + STATE] = cb_ref[
            :, g * STATE : (g + 1) * STATE
        ].astype(F32)
        taps[g, 0:tap_count, group_width + STATE : group_width + 2 * STATE] = cc_ref[
            :, g * STATE : (g + 1) * STATE
        ].astype(F32)

    @pl.when(pos == 0)
    def _():
        s_in[...] = jnp.zeros(s_in.shape, BF16)
        ext[:, 0:8, :] = jnp.zeros((groups, 8, ext.shape[2]), F32)

    for load in loads[1:4]:
        load.wait()
    for copy in shares:
        copy.wait_recv()

    rates = par[0, 0:1, tap_width : tap_width + LANES]
    for s in range(1, sp):
        rates = rates + par[s, 0:1, tap_width : tap_width + LANES]
    log_decay = dt * (-jnp.exp(rates))
    cum = dot(jnp.where(causal, 1.0, 0.0).astype(F32), log_decay, lax.Precision.HIGHEST)
    cum_t = jnp.transpose(cum)
    for chunk in range(inner_width // LANES):
        first = chunk * LANES
        g, at = first // group_width, first % group_width
        s, off = first // tap_width, first % tap_width
        taps[g, 0:tap_count, at : at + LANES] = par[s, 0:tap_count, off : off + LANES]

    @pl.when(pos > 0)
    def _():
        for copy in halos:
            copy.wait_recv()
        for g in range(groups):
            wide = slice(g * group_width, (g + 1) * group_width)
            thin = slice(g * STATE, (g + 1) * STATE)
            ext[g, 0:8, 0:group_width] = halo_x[:, wide].astype(F32)[HALO - 8 :]
            ext[g, 0:8, group_width : group_width + STATE] = halo_b[:, thin].astype(F32)[
                HALO - 8 :
            ]
            ext[g, 0:8, group_width + STATE :] = halo_c[:, thin].astype(F32)[HALO - 8 :]

    left_half = lax.broadcasted_iota(jnp.int32, (tokens, LANES), 1) < HEAD_DIM

    def chain(g):
        return remote(
            s_out.at[g], s_in.at[g], chain_send.at[g], chain_recv.at[g], {"sp": following}
        )

    lag = jnp.minimum(LAG * pos, groups)

    def pass_on(step):
        j = step - lag

        @pl.when((pos > 0) & (pos < sp - 1) & (j >= 0) & (j < groups))
        def _():
            chain(j).wait_recv()
            s_out[j] = (s_in[j].astype(F32) * elast[j, 0:1, :] + local[j]).astype(BF16)
            chain(j).start()

    def conv(g, source, at):
        columns = slice(at, at + LANES)
        ext[g, 8 : 8 + tokens, columns] = source.astype(F32)
        total = taps[g, 0:1, columns] * ext[g, 9 - tap_count : 9 - tap_count + tokens, columns]
        for k in range(1, tap_count):
            start = 9 - tap_count + k
            total = total + taps[g, k : k + 1, columns] * ext[g, start : start + tokens, columns]
        return (total / (1.0 + jnp.exp(-total))).astype(BF16)

    for g in range(groups):
        thin = slice(g * STATE, (g + 1) * STATE)
        b_act = conv(g, b_v[:, thin], group_width)
        c_act = conv(g, c_v[:, thin], group_width + STATE)
        cact[g] = c_act
        b_t = jnp.transpose(b_act)
        scores = dot(c_act, b_t)
        for p in range(pairs):
            at = g * group_width + p * LANES
            columns = slice(at, at + LANES)
            x_act = conv(g, x_v[:, columns], p * LANES).astype(F32)
            h = g * ratio + 2 * p
            spread = [
                jnp.broadcast_to(cum[:, h + i : h + i + 1], (tokens, LANES)) for i in range(2)
            ]
            step = jnp.where(left_half, dt[:, h : h + 1], dt[:, h + 1 : h + 2])
            both = jnp.where(left_half, spread[0], spread[1])
            x_dt = x_act * step
            x_low = x_dt.astype(BF16)
            parts = []
            for i in range(2):
                gap = spread[i] - cum_t[h + i : h + i + 1, :]
                weight = scores * jnp.exp(jnp.where(causal, gap, -jnp.inf))
                parts.append(dot(weight.astype(BF16), x_low))
            inner[:, columns] = jnp.where(left_half, parts[0], parts[1])
            ecum[:, columns] = jnp.exp(both)
            last = both[tokens - 1 : tokens, :]
            elast[g, 0:1, p * LANES : (p + 1) * LANES] = jnp.exp(last)
            x_tail = (x_dt * jnp.exp(last - both)).astype(BF16)
            local[g, :, p * LANES : (p + 1) * LANES] = dot(b_t, x_tail)

        @pl.when(pos == 0)
        def _():
            s_out[g] = local[g].astype(BF16)
            if sp > 1:
                chain(g).start()

        pass_on(g)
        if g == FIRST_AT:
            for way in range(2):
                arrived(way, 0)
            for way, spot in held_back:
                ring_copy(way, spot).start()

    loads[6].wait()
    loads[7].wait()
    sum_down = lax.broadcasted_iota(jnp.int32, (group_width, group_width), 0) // HEAD_DIM
    sum_across = lax.broadcasted_iota(jnp.int32, (group_width, group_width), 1) // HEAD_DIM
    averager = jnp.where(sum_down == sum_across, 1.0 / HEAD_DIM, 0.0).astype(BF16)

    for g in range(groups):
        if share and g == SHARE_AT:
            for way in range(2):
                arrived(way, len(items[way]) - 1)

            @pl.when(mate == 1)
            def _():
                send_shares(False)

            @pl.when(pos == 0)
            def _():
                send_shares(True)

        wide = slice(g * group_width, (g + 1) * group_width)

        pass_on(groups + g)

        @pl.when((pos > 0) & (pos == sp - 1))
        def _():
            chain(g).wait_recv()

        entering = s_in[g]
        core_out = (inner[:, wide] + ecum[:, wide] * dot(cact[g], entering)).astype(BF16)
        gate = z_v[:, wide].astype(F32)
        value = core_out.astype(F32) * (gate / (1.0 + jnp.exp(-gate)))
        square = value * value
        high = square.astype(BF16)
        low = (square - high.astype(F32)).astype(BF16)
        mean = dot(high, averager) + dot(low, averager)
        normed[:, wide] = (value * lax.rsqrt(mean + NORM_EPS) * gain_ref[0:1, wide]).astype(BF16)

    if share:

        @pl.when((mate == 0) & (pos > 0))
        def _():
            send_shares(True)

    keep.wait()
    own.wait_recv()
    aligned = rows % LANES == 0

    def project(offset, first):
        chip = snake((ring_at + offset + chips) % chips)
        start = pl.multiple_of(chip * 2 * rows, 2 * rows)
        part = dot(normed[:, pl.ds(start, 2 * rows)], w_all[pl.ds(start, 2 * rows), :])
        if first:
            acc[...] = part
        else:
            acc[...] += part

    if aligned:
        project(0, True)
    last_spot = len(items[0]) - 1
    for spot in range(1, last_spot + (0 if share else 1)):
        for way in range(2):
            arrived(way, spot)
    if share:
        for up in (False, True):

            @pl.when(mate == (1 if up else 0))
            def _():
                for way in range(2):
                    share_copy(up, way).wait_recv()
                    share_relay(way).start()

    for spot in range(last_spot + 1):
        for way in range(2):
            relay_copy(way, spot).wait_recv()
    if share:
        for way in range(2):
            share_relay(way).wait_recv()

    if aligned:
        for offset in range(1, chips):
            project(offset, False)
        out_ref[0] = acc[...].astype(BF16)
    else:
        out_ref[0] = dot(normed[...], w_all[...]).astype(BF16)

    own.wait_send()
    for copy in shares:
        copy.wait_send()
    for way in range(2):
        for spot in range(last_spot + 1):
            ring_copy(way, spot).wait_send()
            relay_copy(way, spot).wait_send()
    if share:
        for way in range(2):
            share_relay(way).wait_send()
        for up in (False, True):

            @pl.when(mate == (0 if up else 1))
            def _():
                for way in range(2):
                    share_copy(up, way).wait_send()

    @pl.when(pos < sp - 1)
    def _():
        for copy in halos:
            copy.wait_send()
        for g in range(groups):
            chain(g).wait_send()


def body(
    sp,
    dp,
    stream_x,
    stream_b,
    stream_c,
    gate_z,
    step_raw,
    conv_x,
    conv_b,
    conv_c,
    decay_log,
    norm_gain,
    w_out,
):
    tokens, width = stream_x.shape[1:]
    state_width = stream_b.shape[2]
    groups = state_width // STATE
    group_width = width // groups
    columns = w_out.shape[1]
    spots = len(ring_items(sp, dp // 2, w_out.shape[0] // 2)[0][0])
    vmem = pl.BlockSpec(memory_space=pltpu.VMEM)
    anywhere = pl.BlockSpec(memory_space=pl.ANY)
    dma = pltpu.SemaphoreType.DMA
    return pl.pallas_call(
        functools.partial(kernel, sp, dp),
        out_shape=pltpu.VMEM((1, tokens, columns), BF16),
        in_specs=[anywhere] * 4 + [vmem] + [anywhere] * 3 + [vmem] + [anywhere] * 2,
        out_specs=vmem,
        scratch_shapes=[
            pltpu.VMEM(conv_x.shape, BF16),
            pltpu.VMEM(conv_b.shape, BF16),
            pltpu.VMEM(conv_c.shape, BF16),
            pltpu.VMEM((1, width), F32),
            pltpu.VMEM((tokens, width), BF16),
            pltpu.VMEM((tokens, state_width), BF16),
            pltpu.VMEM((tokens, state_width), BF16),
            pltpu.VMEM((tokens, width), BF16),
            pltpu.VMEM((HALO, width), BF16),
            pltpu.VMEM((HALO, state_width), BF16),
            pltpu.VMEM((HALO, state_width), BF16),
            pltpu.VMEM((sp, 8, conv_x.shape[1] + LANES), F32),
            pltpu.VMEM((groups, 8, group_width + 2 * STATE), F32),
            pltpu.VMEM((LANES, tokens), F32),
            pltpu.VMEM((groups, tokens + 8, group_width + 2 * STATE), F32),
            pltpu.VMEM((tokens, width), F32),
            pltpu.VMEM((tokens, width), F32),
            pltpu.VMEM((groups, 8, group_width), F32),
            pltpu.VMEM((groups, tokens, STATE), BF16),
            pltpu.VMEM((groups, STATE, group_width), F32),
            pltpu.VMEM((groups, STATE, group_width), BF16),
            pltpu.VMEM((groups, STATE, group_width), BF16),
            pltpu.VMEM((tokens, width), BF16),
            pltpu.VMEM((width, columns), BF16),
            pltpu.VMEM((tokens, columns), F32),
            dma((9,)),
            dma((max(1, sp - 1),)),
            dma((max(1, sp - 1),)),
            dma((3,)),
            dma((3,)),
            dma((groups,)),
            dma((groups,)),
            dma((2,)),
            dma((2, spots)),
            dma((2, spots)),
            dma((2, spots)),
            dma((2, spots)),
            dma((2, 2)),
            dma((2, 2)),
            dma((2,)),
            dma((2,)),
        ],
        compiler_params=pltpu.CompilerParams(
            collective_id=0, has_side_effects=True, vmem_limit_bytes=60 * 1024 * 1024
        ),
    )(
        stream_x,
        stream_b,
        stream_c,
        gate_z,
        jnp.swapaxes(step_raw, 1, 2),
        conv_x,
        conv_b,
        conv_c,
        decay_log.reshape(1, -1),
        norm_gain.reshape(1, -1),
        w_out,
    )


def solution(mesh):
    placed = (
        P("dp", "sp", None),
        P("dp", "sp", None),
        P("dp", "sp", None),
        P("dp", "sp", None),
        P("dp", "sp", None),
        P(None, "sp"),
        P(),
        P(),
        P("sp"),
        P(),
        P("dp", None),
    )
    return jax.shard_map(
        functools.partial(body, mesh.shape["sp"], mesh.shape["dp"]),
        mesh=mesh,
        in_specs=placed,
        out_specs=P("dp", "sp", None),
        check_vma=False,
    )
```
